32 devices in a mesh: sp: 16 (over z, y, core), tp: 2 (over x).
Axes of the slice: x: 2, y: 2, z: 4, core: 2. Of those that a mesh axis runs over, the one named last changes fastest.
Arguments:
- inputs: bfloat16 [4096, 4096], P('sp', 'tp'), may hold values from -20 to 20
- norm_gain: float32 [3, 4096], replicated, may hold values from 0.1 to 1.9
- in_weight: bfloat16 [3, 4096, 1024], P(None, 'tp', 'sp'), may hold values from -0.09375 to 0.09375
- pool_scale: float32 [3, 1024], replicated, may hold values from 0.1 to 1.9
- out_weight: bfloat16 [3, 1024, 4096], P(None, 'sp', 'tp'), may hold values from -0.1875 to 0.1875
Outputs:
- final_state: bfloat16 [4096, 4096], P('sp', 'tp')
The draws below stay inside these ranges and needn't reach their ends.
All inputs are finite; a program needn't handle non-finite values.
Results may differ from the reference program's by a relative error of at most 0.017.
Values may be sent and summed in bfloat16 or wider, within the bound.
No kernel may reach another device: no remote copies, remote signals or barrier semaphores. Data moves between devices by JAX's collectives and lax.ppermute only.
A program may use at most 64 MiB of HBM per device.

```python
import jax
import jax.numpy as jnp
from jax import lax

D = 4096
P_SIZE = 1024
LAYERS = 3
TOKENS = 4096


def draw_inputs(key, part):
    column = lax.broadcasted_iota(jnp.float32, (1, D), 1) / D
    rough = jax.random.uniform(jax.random.fold_in(key, 2), (1, D), jnp.float32, 0.6, 1.4)
    column_scale = 0.35 * jnp.exp(jnp.log(10.0) * column) * rough
    base = jnp.clip(jax.random.normal(jax.random.fold_in(key, 1), (TOKENS, D), jnp.float32), -4.0, 4.0)
    return jnp.clip(base * column_scale, -20.0, 20.0).astype(jnp.bfloat16)


def levels(own_key, shape, split, least, largest):
    level = 1.0
    for dim, shards_of in split:
        heights = jax.random.uniform(jax.random.fold_in(jax.random.fold_in(own_key, 6), dim), (shards_of,), jnp.float32, least / len(split), largest / len(split))
        level = level * jnp.repeat(jnp.exp(heights), shape[dim] // shards_of).reshape((-1,) + (1,) * (len(shape) - 1 - dim))
    return level


def centred(own_key, extent, deviation, reach, pieces=(), dtype=jnp.bfloat16):
    values = jax.random.normal(own_key, extent, jnp.float32) * deviation
    if len(pieces) > 0:
        values = levels(own_key, extent, pieces, -0.22, 0.18) * values
    return jnp.clip(values, min=-reach, max=reach).astype(dtype)


def setup_inputs(seed: int = 0) -> dict:
    keys = jax.random.split(jax.random.key(seed), 6)
    inputs = draw_inputs(jax.random.fold_in(keys[5], 71), 0)
    norm_gain = jnp.clip(1.0 + 0.18 * jax.random.normal(keys[1], (LAYERS, D), jnp.float32), 0.1, 1.9)
    in_weight = centred(keys[2], (LAYERS, D, P_SIZE), D ** -0.5, 0.09375, ((1, 2), (2, 16)))
    pool_scale = jnp.clip(1.0 + 0.18 * jax.random.normal(keys[3], (LAYERS, P_SIZE), jnp.float32), 0.1, 1.9)
    out_weight = centred(keys[4], (LAYERS, P_SIZE, D), P_SIZE ** -0.5, 0.1875, ((1, 16), (2, 2)))
    return {"inputs": inputs, "norm_gain": norm_gain, "in_weight": in_weight, "pool_scale": pool_scale, "out_weight": out_weight}


epsilon = 1e-06
halo_rows = 16
group_count = 4

def window_means(extended, row_count, first_channel, first_pos, pool_total):
    width = extended.shape[1]
    channel = first_channel + lax.broadcasted_iota(jnp.int32, (1, width), 1)
    group_index = channel // (pool_total // group_count)
    window_len = jnp.left_shift(jnp.int32(2), group_index)
    running = jnp.zeros((row_count, width), jnp.float32)
    for offset in range(halo_rows):
        shifted = extended[halo_rows - offset:halo_rows - offset + row_count]
        running = running + jnp.where(offset < window_len, shifted, 0.0)
    position = first_pos + lax.broadcasted_iota(jnp.int32, (row_count, 1), 0)
    divisor = jnp.minimum(position + 1, window_len).astype(jnp.float32)
    return running / divisor - extended[halo_rows:]

def reference(inputs, norm_gain, in_weight, pool_scale, out_weight):
    current = inputs
    for layer_index in range(LAYERS):
        widened = current.astype(jnp.float32)
        inv_rms = lax.rsqrt(lax.optimization_barrier(jnp.mean(widened * widened, axis=1, keepdims=True)) + epsilon)
        normed = (widened * inv_rms * norm_gain[layer_index]).astype(jnp.bfloat16)
        pool_in = jnp.dot(normed, in_weight[layer_index], preferred_element_type=jnp.float32).astype(jnp.bfloat16)
        extended = jnp.concatenate([jnp.zeros((halo_rows, P_SIZE), jnp.float32), pool_in.astype(jnp.float32)], 0)
        means = window_means(extended, TOKENS, 0, 0, P_SIZE)
        mixed = (means * pool_scale[layer_index]).astype(jnp.bfloat16)
        branch = jnp.dot(mixed, out_weight[layer_index], preferred_element_type=jnp.float32)
        current = (widened + branch).astype(jnp.bfloat16)
    return current
```

```python
import functools
import math

import jax
import jax.numpy as jnp
import numpy as np
from jax import lax
from jax.experimental import pallas as pl
from jax.experimental.pallas import tpu as pltpu
from jax.sharding import PartitionSpec as P

epsilon = 1e-06
window = 16
group_count = 4
lanes = 128
row_tile = 16


VMEM = pl.BlockSpec(memory_space=pltpu.VMEM)
SMEM = pl.BlockSpec(memory_space=pltpu.SMEM)
ANY = pl.BlockSpec(memory_space=pl.ANY)


def move(value, axis, target):
    pairs = [(s, target(s)) for s in range(lax.axis_size(axis))]
    return lax.ppermute(value, axis, [(s, t) for s, t in pairs if t is not None])


def order_table(nz):
    if nz == 4:
        return [[0, 1, 2, 3], [1, 0, 2, 3], [2, 3, 1, 0], [3, 2, 1, 0]]
    table = [[z] for z in range(nz)]
    bit = 1
    while bit < nz:
        table = [table[z] + table[z ^ bit] for z in range(nz)]
        bit *= 2
    return table


def gather(own, nz, y_first):
    across = lambda v: move(v, "sp", lambda s: s ^ 2)
    if nz != 4:
        bit = 1
        while bit < nz:
            own = jnp.concatenate([own, move(own, "sp", lambda s: s ^ (4 * bit))], 0)
            bit *= 2
        return [(own, list(range(nz))), (across(own), list(range(nz, 2 * nz)))]
    near = jnp.concatenate([own, move(own, "sp", lambda s: s ^ 4)], 0)
    if y_first:
        near = jnp.concatenate([near, across(near)], 0)
    z = lax.axis_index("sp") // 4
    middle = move(near, "sp", lambda s: s ^ 12 if s // 4 in (1, 2) else None)
    ends = move(middle, "sp", lambda s: s ^ 4 if s // 4 in (1, 2) else None)
    far = jnp.where((z == 1) | (z == 2), middle, ends)
    if y_first:
        return [(near, [0, 1, 4, 5]), (far, [2, 3, 6, 7])]
    return [(near, [0, 1]), (far, [2, 3]), (across(near), [4, 5]), (across(far), [6, 7])]


def load_weight(pieces, refs, part, parts, shard, w, sems):
    copies = []
    for (_, places), ref in zip(pieces, refs):
        for k, place in enumerate(places):
            copies.append(
                pltpu.make_async_copy(
                    ref.at[pl.ds((k * parts + part) * shard, shard)],
                    w.at[pl.ds(place * shard, shard)],
                    sems.at[len(copies)],
                )
            )
    for copy in copies:
        copy.start()
    return copies


def in_kernel(first, pieces, part, parts, shard, *refs):
    refs = list(refs)
    state = refs.pop(0)
    deltas = [] if first else [refs.pop(0), refs.pop(0)]
    arrays = [refs.pop(0) for _ in pieces]
    fresh = state if first else refs.pop(0)
    out, squares, w, sq, sems = refs
    copies = load_weight(pieces, arrays, part, parts, shard, w, sems)
    rows = state.shape[0]
    tile = 5 * row_tile if rows % (5 * row_tile) == 0 else row_tile

    @pl.loop(0, rows // tile)
    def _(i):
        at = pl.ds(pl.multiple_of(i * tile, row_tile), tile)
        value = state[at, :].astype(jnp.float32)
        if not first:
            value = value + (deltas[0][at, :].astype(jnp.float32) + deltas[1][at, :].astype(jnp.float32))
            rounded = value.astype(jnp.bfloat16)
            fresh[at, :] = rounded
            value = rounded.astype(jnp.float32)
        total = jnp.sum(value * value, axis=1, keepdims=True)
        sq[at, :] = jnp.broadcast_to(total, (tile, lanes))

    if rows < sq.shape[0]:
        sq[rows:, :] = jnp.zeros((sq.shape[0] - rows, lanes), jnp.float32)
    squares[...] = sq[...].T[: squares.shape[0], :]
    for copy in copies:
        copy.wait()
    step = min(256, w.shape[0])
    for n in range(0, w.shape[0], step):
        out[:, n : n + step] = lax.dot_general(
            fresh[...], w[n : n + step, :], (((1,), (1,)), ((), ())), preferred_element_type=jnp.float32
        ).astype(jnp.bfloat16)


def out_kernel(last, pieces, part, parts, shard, features, halo, *refs):
    refs = list(refs)
    place, own, other, sq_own, sq_other, group, scale = [refs.pop(0) for _ in range(7)]
    arrays = [refs.pop(0) for _ in pieces]
    outs = [refs.pop(0) for _ in range(2 if last else 1)]
    w, mixed, sems = refs
    copies = load_weight(pieces, arrays, part, parts, shard, w, sems)
    rows, width = own.shape
    inv = lax.rsqrt((sq_own[...] + sq_other[...]) / features + epsilon)
    inv = jnp.broadcast_to(inv[:1, :], (lanes, inv.shape[1])).T[:rows, :]
    position = place[0] - halo + lax.broadcasted_iota(jnp.int32, (rows, lanes), 0)
    inv = jnp.where(position >= 0, inv, 0.0)
    for n in range(0, width, lanes):
        at = slice(n, n + lanes)
        value = (own[:, at].astype(jnp.float32) + other[:, at].astype(jnp.float32)) * inv
        value = value.astype(jnp.bfloat16).astype(jnp.float32)
        kind = jnp.broadcast_to(group[:1, at], (rows, lanes))
        sums, running, shift = [], value, 1
        while shift < window:
            running = running + pltpu.roll(running, shift, 0)
            sums.append(running)
            shift *= 2
        total = sums[-1]
        for g in range(group_count - 1):
            total = jnp.where(kind == g, sums[g], total)
        length = jnp.left_shift(jnp.int32(2), kind)
        divisor = jnp.maximum(jnp.minimum(position + 1, length), 1).astype(jnp.float32)
        means = total / divisor - value
        mixed[:, at] = (means * scale[:1, at]).astype(jnp.bfloat16)
    for copy in copies:
        copy.wait()
    if last:
        count = outs[0].shape[0]
        spans = [halo + place[1] * count, halo + (1 - place[1]) * count]
        takes = [pl.ds(pl.multiple_of(s, row_tile), count) for s in spans]
    else:
        takes = [pl.ds(0, rows)]
    step = min(256, w.shape[1])

    @pl.loop(0, w.shape[1] // step)
    def _(i):
        at = pl.ds(pl.multiple_of(i * step, step), step)
        for out, take in zip(outs, takes):
            out[:, at] = jnp.dot(mixed[take, :], w[:, at], preferred_element_type=jnp.float32).astype(jnp.bfloat16)


def body(inputs, norm_gain, in_weight, pool_scale, out_weight):
    rows, feats = inputs.shape
    layers, _, shard = in_weight.shape
    count = lax.axis_size("sp")
    nz = count // 4
    channels = shard * count
    half = channels // 2
    features = norm_gain.shape[1]
    bf16 = jnp.bfloat16
    here = lax.axis_index("sp")
    core = here % 2

    gain = lax.dynamic_slice_in_dim(norm_gain, lax.axis_index("tp") * feats, feats, 1)
    in_t = (jnp.swapaxes(in_weight, 1, 2).astype(jnp.float32) * gain[:, None, :]).astype(bf16)
    mats = []
    for l in range(layers):
        mats += [in_t[l], out_weight[l]]
    chunks = [[0]] + [[2 * l - 1, 2 * l] for l in range(1, layers)] + [[2 * layers - 1]]
    found = {}
    for chunk in chunks:
        own = jnp.concatenate([mats[m] for m in chunk], 0)
        pieces = gather(own, nz, len(chunk) == 1)
        for k, m in enumerate(chunk):
            found[m] = (pieces, k, len(chunk))

    order = order_table(nz)
    table = [[(order[s // 4][b % nz] * 2 + ((s // 2) % 2 ^ (b // nz))) * 2 + s % 2 for b in range(2 * nz)] for s in range(count)]
    shards = jnp.asarray(np.array(table, np.int32))[here]
    channel = (shards[:, None] * shard + jnp.arange(shard, dtype=jnp.int32)[None, :]).reshape(1, half)
    group = jnp.broadcast_to(channel // (channels // group_count), (8, half))
    scale = pool_scale.reshape(layers, count, shard)[:, shards].reshape(layers, 1, half)
    scale = jnp.broadcast_to(scale, (layers, 8, half))
    place = jnp.stack([(here // 2) * 2 * rows, core]).astype(jnp.int32)

    halo = math.ceil(layers * (window - 1) / row_tile) * row_tile
    tail = inputs[rows - halo :]
    before = [move(tail, "sp", lambda s, d=d: s + d if s % 2 == 1 and s + d < count else None) for d in (1, 2)]
    sibling = move(inputs, "sp", lambda s: s ^ 1)
    low = core == 0
    state = jnp.concatenate(
        [jnp.where(low, *before), jnp.where(low, inputs, sibling), jnp.where(low, sibling, inputs)], 0
    )
    total = state.shape[0]
    padded = math.ceil(total / lanes) * lanes
    shape = jax.ShapeDtypeStruct
    params = pltpu.CompilerParams(vmem_limit_bytes=48 * 2**20)
    flops = 2 * total * feats * half
    cost = pl.CostEstimate(flops=flops, bytes_accessed=2 * (half * feats + 3 * total * feats), transcendentals=0)

    deltas = []
    for l in range(layers):
        first, last = l == 0, l == layers - 1
        pieces, k, n = found[2 * l]
        outs = [shape((total, half), bf16), shape((8, padded), jnp.float32)]
        if not first:
            outs = [shape((total, feats), bf16)] + outs
        results = pl.pallas_call(
            functools.partial(in_kernel, first, pieces, k, n, shard),
            out_shape=outs,
            in_specs=[VMEM] * (1 if first else 3) + [ANY] * len(pieces),
            out_specs=[VMEM] * len(outs),
            scratch_shapes=[
                pltpu.VMEM((half, feats), bf16),
                pltpu.VMEM((padded, lanes), jnp.float32),
                pltpu.SemaphoreType.DMA((2 * nz,)),
            ],
            compiler_params=params,
            cost_estimate=cost,
            name=f"project_in_{l}",
        )(state, *deltas, *[a for a, _ in pieces])
        if not first:
            state = results[0]
        partial, squares = results[-2:]
        bit = lax.axis_size("tp") // 2
        while True:
            others = [move(v, "tp", lambda s: s ^ bit) for v in (partial, squares)]
            bit //= 2
            if bit == 0:
                break
            partial, squares = partial + others[0], squares + others[1]
        pieces, k, n = found[2 * l + 1]
        outs = [shape((rows if last else total, feats), bf16)] * (2 if last else 1)
        results = pl.pallas_call(
            functools.partial(out_kernel, last, pieces, k, n, shard, features, halo),
            out_shape=outs,
            in_specs=[SMEM] + [VMEM] * 6 + [ANY] * len(pieces),
            out_specs=[VMEM] * len(outs),
            scratch_shapes=[
                pltpu.VMEM((half, feats), bf16),
                pltpu.VMEM((total, half), bf16),
                pltpu.SemaphoreType.DMA((2 * nz,)),
            ],
            compiler_params=params,
            cost_estimate=cost,
            name=f"project_out_{l}",
        )(place, partial, others[0], squares, others[1], group, scale[l], *[a for a, _ in pieces])
        deltas = [results[0], move(results[-1], "sp", lambda s: s ^ 1)]

    own = lax.dynamic_slice_in_dim(state, halo + core * rows, rows, 0)
    return (own.astype(jnp.float32) + (deltas[0].astype(jnp.float32) + deltas[1].astype(jnp.float32))).astype(bf16)


def solution(mesh):
    placed = (P("sp", "tp"), P(), P(None, "tp", "sp"), P(), P(None, "sp", "tp"))
    return jax.shard_map(body, mesh=mesh, in_specs=placed, out_specs=P("sp", "tp"), check_vma=False)
```

```python
import functools
import math

import jax
import jax.numpy as jnp
import numpy as np
from jax import lax
from jax.experimental import pallas as pl
from jax.experimental.pallas import tpu as pltpu
from jax.sharding import PartitionSpec as P


epsilon = 1e-06
early_pieces = ()
window = 16
group_count = 4
lanes = 128
row_tile = 16


VMEM = pl.BlockSpec(memory_space=pltpu.VMEM)
SMEM = pl.BlockSpec(memory_space=pltpu.SMEM)
ANY = pl.BlockSpec(memory_space=pl.ANY)


def move(value, axis, target):
    pairs = [(s, target(s)) for s in range(lax.axis_size(axis))]
    return lax.ppermute(value, axis, [(s, t) for s, t in pairs if t is not None])


def levels(nz):
    return [1 << b for b in range(nz.bit_length() - 1)]


def next_hop(z, m, step):
    at = z % (2 * m)
    if step == 0:
        return z + 1 if at == m - 1 else z - 1 if at == m else None
    return z - 1 if at == m - step else z + 1 if at == m - 1 + step else None


def order_table(nz):
    table = [[z] for z in range(nz)]
    for m in levels(nz):
        edge = lambda z: z - z % (2 * m) + (m if z % (2 * m) < m else m - 1)
        table = [table[z] + table[edge(z)] for z in range(nz)]
    return table


def hop(value, m, step):
    def target(s):
        z = next_hop(s // 4, m, step)
        return None if z is None else 4 * z + s % 4

    return move(value, "sp", target)


def gather(own, nz, split, early):
    across = lambda v: move(v, "sp", lambda s: s ^ 2)
    beyond = lambda at: [p + nz for p in at]
    join = lambda parts: [(jnp.concatenate([v for v, _ in parts], 0), sum([at for _, at in parts], []))]
    z = lax.axis_index("sp") // 4
    pieces = [(own, [0])]
    for m in levels(nz):
        last = 2 * m == nz
        if early and last:
            pieces = join(pieces + [(across(v), beyond(at)) for v, at in pieces])
        arrived = []
        for v, at in pieces:
            steps = z % (2 * m)
            steps = jnp.where(steps < m, m - 1 - steps, steps - m)
            far = got = hop(v, m, 0)
            for t in range(1, m):
                got = hop(got, m, t)
                far = jnp.where(steps == t, got, far)
            arrived.append((far, [q + m for q in at]))
        pieces = pieces + arrived
        if not split and not last:
            pieces = join(pieces)
    if not early:
        pieces = pieces + [(across(v), beyond(at)) for v, at in pieces]
    return pieces


def load_weight(pieces, refs, shard, w, sems):
    copies = []
    for (_, places), ref in zip(pieces, refs):
        for k, place in enumerate(places):
            copies.append(
                pltpu.make_async_copy(
                    ref.at[pl.ds(k * shard, shard)],
                    w.at[pl.ds(place * shard, shard)],
                    sems.at[len(copies)],
                )
            )
    for copy in copies:
        copy.start()
    return copies


def in_kernel(first, pieces, shard, *refs):
    refs = list(refs)
    state = refs.pop(0)
    deltas = [] if first else [refs.pop(0), refs.pop(0)]
    arrays = [refs.pop(0) for _ in pieces]
    fresh = state if first else refs.pop(0)
    out, squares, w, sq, sems = refs
    copies = load_weight(pieces, arrays, shard, w, sems)
    rows = state.shape[0]
    tile = 5 * row_tile if rows % (5 * row_tile) == 0 else row_tile

    @pl.loop(0, rows // tile)
    def _(i):
        at = pl.ds(pl.multiple_of(i * tile, row_tile), tile)
        value = state[at, :].astype(jnp.float32)
        if not first:
            value = value + (deltas[0][at, :].astype(jnp.float32) + deltas[1][at, :].astype(jnp.float32))
            rounded = value.astype(jnp.bfloat16)
            fresh[at, :] = rounded
            value = rounded.astype(jnp.float32)
        total = jnp.sum(value * value, axis=1, keepdims=True)
        sq[at, :] = jnp.broadcast_to(total, (tile, lanes))

    if rows < sq.shape[0]:
        sq[rows:, :] = jnp.zeros((sq.shape[0] - rows, lanes), jnp.float32)
    squares[...] = sq[...].T[: squares.shape[0], :]
    for copy in copies:
        copy.wait()
    step = min(256, w.shape[0])
    for n in range(0, w.shape[0], step):
        out[:, n : n + step] = lax.dot_general(
            fresh[...], w[n : n + step, :], (((1,), (1,)), ((), ())), preferred_element_type=jnp.float32
        ).astype(jnp.bfloat16)


def out_kernel(last, pieces, shard, features, halo, *refs):
    refs = list(refs)
    place, own, other, sq_own, sq_other, group, scale = [refs.pop(0) for _ in range(7)]
    arrays = [refs.pop(0) for _ in pieces]
    outs = [refs.pop(0) for _ in range(2 if last else 1)]
    w, mixed, sems = refs
    copies = load_weight(pieces, arrays, shard, w, sems)
    rows, width = own.shape
    inv = lax.rsqrt((sq_own[...] + sq_other[...]) / features + epsilon)
    inv = jnp.broadcast_to(inv[:1, :], (lanes, inv.shape[1])).T[:rows, :]
    position = place[0] - halo + lax.broadcasted_iota(jnp.int32, (rows, lanes), 0)
    inv = jnp.where(position >= 0, inv, 0.0)
    for n in range(0, width, lanes):
        at = slice(n, n + lanes)
        value = (own[:, at].astype(jnp.float32) + other[:, at].astype(jnp.float32)) * inv
        value = value.astype(jnp.bfloat16).astype(jnp.float32)
        kind = jnp.broadcast_to(group[:1, at], (rows, lanes))
        sums, running, shift = [], value, 1
        while shift < window:
            running = running + pltpu.roll(running, shift, 0)
            sums.append(running)
            shift *= 2
        total = sums[-1]
        for g in range(group_count - 1):
            total = jnp.where(kind == g, sums[g], total)
        length = jnp.left_shift(jnp.int32(2), kind)
        divisor = jnp.maximum(jnp.minimum(position + 1, length), 1).astype(jnp.float32)
        means = total / divisor - value
        mixed[:, at] = (means * scale[:1, at]).astype(jnp.bfloat16)
    for copy in copies:
        copy.wait()
    if last:
        count = outs[0].shape[0]
        spans = [halo + place[1] * count, halo + (1 - place[1]) * count]
        takes = [pl.ds(pl.multiple_of(s, row_tile), count) for s in spans]
    else:
        takes = [pl.ds(0, rows)]
    step = min(256, w.shape[1])

    @pl.loop(0, w.shape[1] // step)
    def _(i):
        at = pl.ds(pl.multiple_of(i * step, step), step)
        for out, take in zip(outs, takes):
            out[:, at] = jnp.dot(mixed[take, :], w[:, at], preferred_element_type=jnp.float32).astype(jnp.bfloat16)


def body(inputs, norm_gain, in_weight, pool_scale, out_weight):
    rows, feats = inputs.shape
    layers, _, shard = in_weight.shape
    count = lax.axis_size("sp")
    nz = count // 4
    channels = shard * count
    half = channels // 2
    features = norm_gain.shape[1]
    bf16 = jnp.bfloat16
    here = lax.axis_index("sp")
    core = here % 2

    gain = lax.dynamic_slice_in_dim(norm_gain, lax.axis_index("tp") * feats, feats, 1)
    in_t = (jnp.swapaxes(in_weight, 1, 2).astype(jnp.float32) * gain[:, None, :]).astype(bf16)
    mats = []
    for l in range(layers):
        mats += [in_t[l], out_weight[l]]
    found = {}
    for m, own in enumerate(mats):
        found[m] = gather(own, nz, m == 0, m in early_pieces)

    order = order_table(nz)
    table = [[(order[s // 4][b % nz] * 2 + ((s // 2) % 2 ^ (b // nz))) * 2 + s % 2 for b in range(2 * nz)] for s in range(count)]
    shards = jnp.asarray(np.array(table, np.int32))[here]
    channel = (shards[:, None] * shard + jnp.arange(shard, dtype=jnp.int32)[None, :]).reshape(1, half)
    group = jnp.broadcast_to(channel // (channels // group_count), (8, half))
    scale = pool_scale.reshape(layers, count, shard)[:, shards].reshape(layers, 1, half)
    scale = jnp.broadcast_to(scale, (layers, 8, half))
    place = jnp.stack([(here // 2) * 2 * rows, core]).astype(jnp.int32)

    halo = math.ceil(layers * (window - 1) / row_tile) * row_tile
    tail = inputs[rows - halo :]
    reach = lambda d: move(tail, "sp", lambda s: s + d if s % 2 == 1 and s + d < count else None)
    before = [reach(d) for d in (1, 2)]
    sibling = move(inputs, "sp", lambda s: s ^ 1)
    low = core == 0
    state = jnp.concatenate(
        [jnp.where(low, *before), jnp.where(low, inputs, sibling), jnp.where(low, sibling, inputs)], 0
    )
    total = state.shape[0]
    padded = math.ceil(total / lanes) * lanes
    shape = jax.ShapeDtypeStruct
    params = pltpu.CompilerParams(vmem_limit_bytes=24 * 2**20)
    flops = 2 * total * feats * half
    cost = pl.CostEstimate(flops=flops, bytes_accessed=2 * (half * feats + 3 * total * feats), transcendentals=0)

    deltas = []
    for l in range(layers):
        first, last = l == 0, l == layers - 1
        pieces = found[2 * l]
        outs = [shape((total, half), bf16), shape((8, padded), jnp.float32)]
        if not first:
            outs = [shape((total, feats), bf16)] + outs
        results = pl.pallas_call(
            functools.partial(in_kernel, first, pieces, shard),
            out_shape=outs,
            in_specs=[VMEM] * (1 if first else 3) + [ANY] * len(pieces),
            out_specs=[VMEM] * len(outs),
            scratch_shapes=[
                pltpu.VMEM((half, feats), bf16),
                pltpu.VMEM((padded, lanes), jnp.float32),
                pltpu.SemaphoreType.DMA((2 * nz,)),
            ],
            compiler_params=params,
            cost_estimate=cost,
        )(state, *deltas, *[a for a, _ in pieces])
        if not first:
            state = results[0]
        partial, squares = results[-2:]
        bits = levels(lax.axis_size("tp"))
        for b, bit in enumerate(bits):
            swap = lambda v: move(v, "tp", lambda s: s ^ bit)
            others = [swap(partial), swap(squares)]
            if b < len(bits) - 1:
                partial, squares = partial + others[0], squares + others[1]
        pieces = found[2 * l + 1]
        outs = [shape((rows if last else total, feats), bf16)] * (2 if last else 1)
        results = pl.pallas_call(
            functools.partial(out_kernel, last, pieces, shard, features, halo),
            out_shape=outs,
            in_specs=[SMEM] + [VMEM] * 6 + [ANY] * len(pieces),
            out_specs=[VMEM] * len(outs),
            scratch_shapes=[
                pltpu.VMEM((half, feats), bf16),
                pltpu.VMEM((total, half), bf16),
                pltpu.SemaphoreType.DMA((2 * nz,)),
            ],
            compiler_params=params,
            cost_estimate=cost,
        )(place, partial, others[0], squares, others[1], group, scale[l], *[a for a, _ in pieces])
        deltas = [results[0], move(results[-1], "sp", lambda s: s ^ 1)]

    own = lax.dynamic_slice_in_dim(state, halo + core * rows, rows, 0)
    return (own.astype(jnp.float32) + (deltas[0].astype(jnp.float32) + deltas[1].astype(jnp.float32))).astype(bf16)


def solution(mesh):
    placed = (P("sp", "tp"), P(), P(None, "tp", "sp"), P(), P(None, "sp", "tp"))

    return jax.shard_map(body, mesh=mesh, in_specs=placed, out_specs=P("sp", "tp"), check_vma=False)
```

```python
import functools
import math

import jax
import jax.numpy as jnp
import numpy as np
from jax import lax
from jax.experimental import pallas as pl
from jax.experimental.pallas import tpu as pltpu
from jax.sharding import PartitionSpec as P


epsilon = 1e-06
window = 16
group_count = 4
lanes = 128
row_tile = 16


VMEM = pl.BlockSpec(memory_space=pltpu.VMEM)
SMEM = pl.BlockSpec(memory_space=pltpu.SMEM)
ANY = pl.BlockSpec(memory_space=pl.ANY)
HBM = pl.BlockSpec(memory_space=pltpu.HBM)


def move(value, axis, target):
    pairs = [(s, target(s)) for s in range(lax.axis_size(axis))]
    return lax.ppermute(value, axis, [(s, t) for s, t in pairs if t is not None])


def levels(nz):
    return [1 << b for b in range(nz.bit_length() - 1)]


def next_hop(z, m, step):
    at = z % (2 * m)
    if step == 0:
        return z + 1 if at == m - 1 else z - 1 if at == m else None
    return z - 1 if at == m - step else z + 1 if at == m - 1 + step else None


def order_table(nz):
    table = [[z] for z in range(nz)]
    for m in levels(nz):
        edge = lambda z: z - z % (2 * m) + (m if z % (2 * m) < m else m - 1)
        table = [table[z] + table[edge(z)] for z in range(nz)]
    return table


def across(value):
    return move(value, "sp", lambda s: s ^ 2)


def level(value, m):
    at = lax.axis_index("sp") // 4 % (2 * m)
    steps = jnp.where(at < m, m - 1 - at, at - m)

    def hop(v, step):
        def target(s):
            z = next_hop(s // 4, m, step)
            return None if z is None else 4 * z + s % 4

        return move(v, "sp", target)

    far = got = hop(value, 0)
    for t in range(1, m):
        got = hop(got, t)
        far = jnp.where(steps == t, got, far)
    return far


def lower(stack, nz):
    arrived, near = [], stack
    for m in levels(nz)[:-1]:
        far = level(near, m)
        arrived.append((far, list(range(m, 2 * m))))
        near = jnp.concatenate([near, far], 1)
    return arrived


def gather(own, opposite, arrived, crossed, nz, split):
    half = nz // 2
    pick = lambda e: e[0] if e[2] is None else e[0][e[2]]
    join = lambda parts: (jnp.concatenate([pick(e) for e in parts], 0), sum([e[1] for e in parts], []), None)
    near = [(own, [0], None)] + arrived
    beyond = [opposite] + crossed
    if not split:
        near = [join(near)]
    far = [(level(pick(e), half), [q + half for q in e[1]], None) for e in near]
    return near + far + beyond + [(across(v), [q + nz for q in at], None) for v, at, _ in far]


def load_weight(pieces, refs, shard, w, sems):
    copies = []
    for (places, index), ref in zip(pieces, refs):
        for k, place in enumerate(places):
            rows = pl.ds(k * shard, shard)
            copies.append(
                pltpu.make_async_copy(
                    ref.at[rows] if index is None else ref.at[index, rows],
                    w.at[pl.ds(place * shard, shard)],
                    sems.at[len(copies)],
                )
            )
    for copy in copies:
        copy.start()
    return copies


def in_kernel(first, pieces, shard, *refs):
    refs = list(refs)
    state = refs.pop(0)
    deltas = [] if first else [refs.pop(0), refs.pop(0)]
    arrays = [refs.pop(0) for _ in pieces]
    kept = None if first else refs.pop(0)
    out, squares, w, sq, sems = refs[:5]
    fresh = state if first else refs[5]
    copies = load_weight(pieces, arrays, shard, w, sems)
    rows = state.shape[0]
    tile = 5 * row_tile if rows % (5 * row_tile) == 0 else row_tile

    @pl.loop(0, rows // tile)
    def _(i):
        at = pl.ds(pl.multiple_of(i * tile, row_tile), tile)
        value = state[at, :].astype(jnp.float32)
        if not first:
            value = value + (deltas[0][at, :].astype(jnp.float32) + deltas[1][at, :].astype(jnp.float32))
            rounded = value.astype(jnp.bfloat16)
            fresh[at, :] = rounded
            value = rounded.astype(jnp.float32)
        total = jnp.sum(value * value, axis=1, keepdims=True)
        sq[at, :] = jnp.broadcast_to(total, (tile, lanes))

    if not first:
        keep = pltpu.make_async_copy(fresh, kept, refs[6])
        keep.start()
    if rows < sq.shape[0]:
        sq[rows:, :] = jnp.zeros((sq.shape[0] - rows, lanes), jnp.float32)
    squares[...] = sq[...].T[: squares.shape[0], :]
    for copy in copies:
        copy.wait()
    step = min(256, w.shape[0])
    for n in range(0, w.shape[0], step):
        out[:, n : n + step] = lax.dot_general(
            fresh[...], w[n : n + step, :], (((1,), (1,)), ((), ())), preferred_element_type=jnp.float32
        ).astype(jnp.bfloat16)
    if not first:
        keep.wait()


def pool(place, own, other, sq_own, sq_other, group, scale, mixed, features, halo):
    rows, width = own.shape
    inv = lax.rsqrt((sq_own[...] + sq_other[...]) / features + epsilon)
    inv = jnp.broadcast_to(inv[:1, :], (lanes, inv.shape[1])).T[:rows, :]
    position = place[0] - halo + lax.broadcasted_iota(jnp.int32, (rows, lanes), 0)
    inv = jnp.where(position >= 0, inv, 0.0)
    for n in range(0, width, lanes):
        at = slice(n, n + lanes)
        value = (own[:, at].astype(jnp.float32) + other[:, at].astype(jnp.float32)) * inv
        value = value.astype(jnp.bfloat16).astype(jnp.float32)
        kind = jnp.broadcast_to(group[:1, at], (rows, lanes))
        sums, running, shift = [], value, 1
        while shift < window:
            running = running + pltpu.roll(running, shift, 0)
            sums.append(running)
            shift *= 2
        total = sums[-1]
        for g in range(group_count - 1):
            total = jnp.where(kind == g, sums[g], total)
        length = jnp.left_shift(jnp.int32(2), kind)
        divisor = jnp.maximum(jnp.minimum(position + 1, length), 1).astype(jnp.float32)
        means = total / divisor - value
        mixed[:, at] = (means * scale[:1, at]).astype(jnp.bfloat16)


def pool_kernel(features, halo, *refs):
    pool(*refs, features, halo)


def out_kernel(pieces, shard, features, halo, *refs):
    operands, arrays = refs[:7], refs[7 : 7 + len(pieces)]
    out, w, mixed, sems = refs[7 + len(pieces) :]
    copies = load_weight(pieces, arrays, shard, w, sems)
    pool(*operands, mixed, features, halo)
    for copy in copies:
        copy.wait()
    step = min(256, w.shape[1])

    @pl.loop(0, w.shape[1] // step)
    def _(i):
        at = pl.ds(pl.multiple_of(i * step, step), step)
        out[:, at] = jnp.dot(mixed[...], w[:, at], preferred_element_type=jnp.float32).astype(jnp.bfloat16)


def last_kernel(pieces, shard, halo, *refs):
    place, mixed, state = refs[:3]
    arrays = refs[3 : 3 + len(pieces)]
    mine, theirs, w, kept, sems, kept_sem = refs[3 + len(pieces) :]
    copies = load_weight(pieces, arrays, shard, w, sems)
    count = mine.shape[0]
    here, there = [
        pl.ds(pl.multiple_of(halo + c * count, row_tile), count) for c in (place[1], 1 - place[1])
    ]
    keep = pltpu.make_async_copy(state.at[here], kept, kept_sem)
    keep.start()
    for copy in copies + [keep]:
        copy.wait()
    step = min(256, w.shape[1])

    @pl.loop(0, w.shape[1] // step)
    def _(i):
        at = pl.ds(pl.multiple_of(i * step, step), step)
        theirs[:, at] = jnp.dot(mixed[there, :], w[:, at], preferred_element_type=jnp.float32).astype(jnp.bfloat16)
        value = jnp.dot(mixed[here, :], w[:, at], preferred_element_type=jnp.float32)
        mine[:, at] = value + kept[:, at].astype(jnp.float32)


def body(inputs, norm_gain, in_weight, pool_scale, out_weight):
    rows, feats = inputs.shape
    layers, _, shard = in_weight.shape
    count = lax.axis_size("sp")
    nz = count // 4
    channels = shard * count
    half = channels // 2
    features = norm_gain.shape[1]
    bf16 = jnp.bfloat16
    here = lax.axis_index("sp")
    core = here % 2

    gain = lax.dynamic_slice_in_dim(norm_gain, lax.axis_index("tp") * feats, feats, 1)
    in_t = (jnp.swapaxes(in_weight, 1, 2).astype(jnp.float32) * gain[:, None, :]).astype(bf16)
    in_opposite = across(in_t)
    found = [None] * (2 * layers)

    def gather_group(stack, matrices, merged):
        arrived = lower(stack, nz)
        whole = [(across(v), at) for v, at in arrived] if merged else None
        for j, k in enumerate(matrices):
            l = k // 2
            mine = [(v, at, j) for v, at in arrived]
            if merged:
                crossed = [(v, [q + nz for q in at], j) for v, at in whole]
            else:
                crossed = [(across(v[j]), [q + nz for q in at], None) for v, at in arrived]
            opposite = (across(out_weight[l]), [nz], None) if k % 2 else (in_opposite, [nz], l)
            found[k] = gather(stack[j], opposite, mine, crossed, nz, k == 0)

    gather_group(in_t[:1], [0], True)
    gather_group(out_weight[:1], [1], True)
    gather_group(in_t[1:], list(range(2, 2 * layers, 2)), True)
    gather_group(out_weight[1:], list(range(3, 2 * layers, 2)), False)

    order = order_table(nz)
    table = [[(order[s // 4][b % nz] * 2 + ((s // 2) % 2 ^ (b // nz))) * 2 + s % 2 for b in range(2 * nz)] for s in range(count)]
    shards = jnp.asarray(np.array(table, np.int32))[here]
    channel = (shards[:, None] * shard + jnp.arange(shard, dtype=jnp.int32)[None, :]).reshape(1, half)
    group = jnp.broadcast_to(channel // (channels // group_count), (8, half))
    scale = pool_scale.reshape(layers, count, shard)[:, shards].reshape(layers, 1, half)
    scale = jnp.broadcast_to(scale, (layers, 8, half))
    place = jnp.stack([(here // 2) * 2 * rows, core]).astype(jnp.int32)

    halo = math.ceil(layers * (window - 1) / row_tile) * row_tile
    tail = inputs[rows - halo :]
    before = move(tail, "sp", lambda s: s + 2 if s % 2 == 1 and s + 2 < count else None)
    relay = move(before, "sp", lambda s: s - 1 if s % 2 == 1 else None)
    sibling = move(inputs, "sp", lambda s: s ^ 1)
    low = core == 0
    state = jnp.concatenate(
        [jnp.where(low, relay, before), jnp.where(low, inputs, sibling), jnp.where(low, sibling, inputs)], 0
    )
    total = state.shape[0]
    padded = math.ceil(total / lanes) * lanes
    shape = jax.ShapeDtypeStruct
    params = pltpu.CompilerParams(vmem_limit_bytes=16 * 2**20)
    flops = 2 * total * feats * half
    cost = pl.CostEstimate(flops=flops, bytes_accessed=2 * (half * feats + 3 * total * feats), transcendentals=0)

    deltas = []
    for l in range(layers):
        first, last = l == 0, l == layers - 1
        pieces = [(at, index) for _, at, index in found[2 * l]]
        arrays = [v for v, _, _ in found[2 * l]]
        outs = [shape((total, half), bf16), shape((8, padded), jnp.float32)]
        if not first:
            outs = [shape((total, feats), bf16)] + outs
        results = pl.pallas_call(
            functools.partial(in_kernel, first, pieces, shard),
            out_shape=outs,
            in_specs=[VMEM] * (1 if first else 3) + [ANY] * len(pieces),
            out_specs=([] if first else [HBM]) + [VMEM] * 2,
            scratch_shapes=[
                pltpu.VMEM((half, feats), bf16),
                pltpu.VMEM((padded, lanes), jnp.float32),
                pltpu.SemaphoreType.DMA((2 * nz,)),
            ]
            + ([] if first else [pltpu.VMEM((total, feats), bf16), pltpu.SemaphoreType.DMA]),
            compiler_params=params,
            cost_estimate=cost,
        )(state, *deltas, *arrays)
        if not first:
            state = results[0]
        partial, squares = results[-2:]
        bits = levels(lax.axis_size("tp"))
        for b, bit in enumerate(bits):
            swap = lambda v: move(v, "tp", lambda s: s ^ bit)
            others = [swap(partial), swap(squares)]
            if b < len(bits) - 1:
                partial, squares = partial + others[0], squares + others[1]
        pieces = [(at, index) for _, at, index in found[2 * l + 1]]
        arrays = [v for v, _, _ in found[2 * l + 1]]
        operands = (place, partial, others[0], squares, others[1], group, scale[l])
        weights = pltpu.VMEM((half, feats), bf16)
        sems = pltpu.SemaphoreType.DMA((2 * nz,))
        mixed = (total, half)
        call = dict(compiler_params=params, cost_estimate=cost)
        if not last:
            results = [
                pl.pallas_call(
                    functools.partial(out_kernel, pieces, shard, features, halo),
                    out_shape=shape((total, feats), bf16),
                    in_specs=[SMEM] + [VMEM] * 6 + [ANY] * len(pieces),
                    out_specs=VMEM,
                    scratch_shapes=[weights, pltpu.VMEM(mixed, bf16), sems],
                    **call,
                )(*operands, *arrays)
            ]
        else:
            mixed = pl.pallas_call(
                functools.partial(pool_kernel, features, halo),
                out_shape=shape(mixed, bf16),
                in_specs=[SMEM] + [VMEM] * 6,
                out_specs=VMEM,
                **call,
            )(*operands)
            results = pl.pallas_call(
                functools.partial(last_kernel, pieces, shard, halo),
                out_shape=[shape((rows, feats), jnp.float32), shape((rows, feats), bf16)],
                in_specs=[SMEM, VMEM, HBM] + [ANY] * len(pieces),
                out_specs=[VMEM] * 2,
                scratch_shapes=[weights, pltpu.VMEM((rows, feats), bf16), sems, pltpu.SemaphoreType.DMA],
                **call,
            )(place, mixed, state, *arrays)
        deltas = [results[0], move(results[-1], "sp", lambda s: s ^ 1)]

    return (deltas[0] + deltas[1].astype(jnp.float32)).astype(bf16)


def solution(mesh):
    placed = (P("sp", "tp"), P(), P(None, "tp", "sp"), P(), P(None, "sp", "tp"))

    return jax.shard_map(body, mesh=mesh, in_specs=placed, out_specs=P("sp", "tp"), check_vma=False)
```

```python
import functools
import math

import jax
import jax.numpy as jnp
import numpy as np
from jax import lax
from jax.experimental import pallas as pl
from jax.experimental.pallas import tpu as pltpu
from jax.sharding import PartitionSpec as P


epsilon = 1e-06
window = 16
group_count = 4
lanes = 128
row_tile = 16


VMEM = pl.BlockSpec(memory_space=pltpu.VMEM)
SMEM = pl.BlockSpec(memory_space=pltpu.SMEM)
ANY = pl.BlockSpec(memory_space=pl.ANY)
HBM = pl.BlockSpec(memory_space=pltpu.HBM)


def move(value, axis, target):
    pairs = [(s, target(s)) for s in range(lax.axis_size(axis))]
    return lax.ppermute(value, axis, [(s, t) for s, t in pairs if t is not None])


def levels(nz):
    return [1 << b for b in range(nz.bit_length() - 1)]


def next_hop(z, m, step):
    at = z % (2 * m)
    if step == 0:
        return z + 1 if at == m - 1 else z - 1 if at == m else None
    return z - 1 if at == m - step else z + 1 if at == m - 1 + step else None


def order_table(nz):
    table = [[z] for z in range(nz)]
    for m in levels(nz):
        edge = lambda z: z - z % (2 * m) + (m if z % (2 * m) < m else m - 1)
        table = [table[z] + table[edge(z)] for z in range(nz)]
    return table


def across(value):
    return move(value, "sp", lambda s: s ^ 2)


def level(value, m):
    at = lax.axis_index("sp") // 4 % (2 * m)
    steps = jnp.where(at < m, m - 1 - at, at - m)

    def hop(v, step):
        def target(s):
            z = next_hop(s // 4, m, step)
            return None if z is None else 4 * z + s % 4

        return move(v, "sp", target)

    far = got = hop(value, 0)
    for t in range(1, m):
        got = hop(got, t)
        far = jnp.where(steps == t, got, far)
    return far


def lower(stack, nz):
    arrived, near = [], stack
    for m in levels(nz)[:-1]:
        far = level(near, m)
        arrived.append((far, list(range(m, 2 * m))))
        near = jnp.concatenate([near, far], 1)
    return arrived


def gather(own, opposite, arrived, crossed, nz, split):
    half = nz // 2
    pick = lambda e: e[0] if e[2] is None else e[0][e[2]]
    join = lambda parts: (jnp.concatenate([pick(e) for e in parts], 0), sum([e[1] for e in parts], []), None)
    near = [(own, [0], None)] + arrived
    beyond = [opposite] + crossed
    if not split:
        near = [join(near)]
    far = [(level(pick(e), half), [q + half for q in e[1]], None) for e in near]
    return near + far + beyond + [(across(v), [q + nz for q in at], None) for v, at, _ in far]


def load_weight(pieces, refs, shard, w, sems):
    copies = []
    for (places, index), ref in zip(pieces, refs):
        for k, place in enumerate(places):
            rows = pl.ds(k * shard, shard)
            copies.append(
                pltpu.make_async_copy(
                    ref.at[rows] if index is None else ref.at[index, rows],
                    w.at[pl.ds(place * shard, shard)],
                    sems.at[len(copies)],
                )
            )
    for copy in copies:
        copy.start()
    return copies


def in_kernel(first, pieces, shard, *refs):
    refs = list(refs)
    state = refs.pop(0)
    deltas = [] if first else [refs.pop(0), refs.pop(0)]
    arrays = [refs.pop(0) for _ in pieces]
    kept = None if first else refs.pop(0)
    out, squares, w, sq, sems = refs[:5]
    fresh = state if first else refs[5]
    copies = load_weight(pieces, arrays, shard, w, sems)
    rows = state.shape[0]
    tile = 5 * row_tile if rows % (5 * row_tile) == 0 else row_tile

    @pl.loop(0, rows // tile)
    def _(i):
        at = pl.ds(pl.multiple_of(i * tile, row_tile), tile)
        value = state[at, :].astype(jnp.float32)
        if not first:
            value = value + (deltas[0][at, :].astype(jnp.float32) + deltas[1][at, :].astype(jnp.float32))
            rounded = value.astype(jnp.bfloat16)
            fresh[at, :] = rounded
            value = rounded.astype(jnp.float32)
        total = jnp.sum(value * value, axis=1, keepdims=True)
        sq[at, :] = jnp.broadcast_to(total, (tile, lanes))

    if not first:
        keep = pltpu.make_async_copy(fresh, kept, refs[6])
        keep.start()
    if rows < sq.shape[0]:
        sq[rows:, :] = jnp.zeros((sq.shape[0] - rows, lanes), jnp.float32)
    squares[...] = sq[...].T[: squares.shape[0], :]
    for copy in copies:
        copy.wait()
    step = min(256, w.shape[0])
    for n in range(0, w.shape[0], step):
        out[:, n : n + step] = lax.dot_general(
            fresh[...], w[n : n + step, :], (((1,), (1,)), ((), ())), preferred_element_type=jnp.float32
        ).astype(jnp.bfloat16)
    if not first:
        keep.wait()


def pool(place, own, other, sq_own, sq_other, group, scale, mixed, features, halo):
    rows, width = own.shape
    inv = lax.rsqrt((sq_own[...] + sq_other[...]) / features + epsilon)
    inv = jnp.broadcast_to(inv[:1, :], (lanes, inv.shape[1])).T[:rows, :]
    position = place[0] - halo + lax.broadcasted_iota(jnp.int32, (rows, lanes), 0)
    inv = jnp.where(position >= 0, inv, 0.0)
    for n in range(0, width, lanes):
        at = slice(n, n + lanes)
        value = (own[:, at].astype(jnp.float32) + other[:, at].astype(jnp.float32)) * inv
        value = value.astype(jnp.bfloat16).astype(jnp.float32)
        kind = jnp.broadcast_to(group[:1, at], (rows, lanes))
        sums, running, shift = [], value, 1
        while shift < window:
            running = running + pltpu.roll(running, shift, 0)
            sums.append(running)
            shift *= 2
        total = sums[-1]
        for g in range(group_count - 1):
            total = jnp.where(kind == g, sums[g], total)
        length = jnp.left_shift(jnp.int32(2), kind)
        divisor = jnp.maximum(jnp.minimum(position + 1, length), 1).astype(jnp.float32)
        means = total / divisor - value
        mixed[:, at] = (means * scale[:1, at]).astype(jnp.bfloat16)


def pool_kernel(features, halo, *refs):
    pool(*refs, features, halo)


def out_kernel(pieces, shard, features, halo, *refs):
    operands, arrays = refs[:7], refs[7 : 7 + len(pieces)]
    out, w, mixed, sems = refs[7 + len(pieces) :]
    copies = load_weight(pieces, arrays, shard, w, sems)
    pool(*operands, mixed, features, halo)
    for copy in copies:
        copy.wait()
    step = min(256, w.shape[1])

    @pl.loop(0, w.shape[1] // step)
    def _(i):
        at = pl.ds(pl.multiple_of(i * step, step), step)
        out[:, at] = jnp.dot(mixed[...], w[:, at], preferred_element_type=jnp.float32).astype(jnp.bfloat16)


def last_kernel(pieces, shard, halo, *refs):
    place, mixed, state = refs[:3]
    arrays = refs[3 : 3 + len(pieces)]
    mine, theirs, w, kept, sems, kept_sem = refs[3 + len(pieces) :]
    copies = load_weight(pieces, arrays, shard, w, sems)
    count = mine.shape[0]
    here, there = [
        pl.ds(pl.multiple_of(halo + c * count, row_tile), count) for c in (place[1], 1 - place[1])
    ]
    keep = pltpu.make_async_copy(state.at[here], kept, kept_sem)
    keep.start()
    for copy in copies + [keep]:
        copy.wait()
    step = min(256, w.shape[1])

    @pl.loop(0, w.shape[1] // step)
    def _(i):
        at = pl.ds(pl.multiple_of(i * step, step), step)
        theirs[:, at] = jnp.dot(mixed[there, :], w[:, at], preferred_element_type=jnp.float32).astype(jnp.bfloat16)
        value = jnp.dot(mixed[here, :], w[:, at], preferred_element_type=jnp.float32)
        mine[:, at] = value + kept[:, at].astype(jnp.float32)


def body(inputs, norm_gain, in_weight, pool_scale, out_weight):
    rows, feats = inputs.shape
    layers, _, shard = in_weight.shape
    count = lax.axis_size("sp")
    nz = count // 4
    channels = shard * count
    half = channels // 2
    features = norm_gain.shape[1]
    bf16 = jnp.bfloat16
    here = lax.axis_index("sp")
    core = here % 2

    gain = lax.dynamic_slice_in_dim(norm_gain, lax.axis_index("tp") * feats, feats, 1)
    in_t = (jnp.swapaxes(in_weight, 1, 2).astype(jnp.float32) * gain[:, None, :]).astype(bf16)
    in_opposite = across(in_t)
    found = [None] * (2 * layers)

    def gather_group(stack, matrices, merged):
        arrived = lower(stack, nz)
        whole = [(across(v), at) for v, at in arrived] if merged else None
        for j, k in enumerate(matrices):
            l = k // 2
            mine = [(v, at, j) for v, at in arrived]
            if merged:
                crossed = [(v, [q + nz for q in at], j) for v, at in whole]
            else:
                crossed = [(across(v[j]), [q + nz for q in at], None) for v, at in arrived]
            opposite = (across(out_weight[l]), [nz], None) if k % 2 else (in_opposite, [nz], l)
            found[k] = gather(stack[j], opposite, mine, crossed, nz, k == 0)

    gather_group(in_t[:1], [0], True)
    gather_group(out_weight[:1], [1], True)
    gather_group(in_t[1:], list(range(2, 2 * layers, 2)), True)
    gather_group(out_weight[1:], list(range(3, 2 * layers, 2)), False)

    order = order_table(nz)
    table = [[(order[s // 4][b % nz] * 2 + ((s // 2) % 2 ^ (b // nz))) * 2 + s % 2 for b in range(2 * nz)] for s in range(count)]
    shards = jnp.asarray(np.array(table, np.int32))[here]
    channel = (shards[:, None] * shard + jnp.arange(shard, dtype=jnp.int32)[None, :]).reshape(1, half)
    group = jnp.broadcast_to(channel // (channels // group_count), (8, half))
    scale = pool_scale.reshape(layers, count, shard)[:, shards].reshape(layers, 1, half)
    scale = jnp.broadcast_to(scale, (layers, 8, half))
    place = jnp.stack([(here // 2) * 2 * rows, core]).astype(jnp.int32)

    halo = math.ceil(layers * (window - 1) / row_tile) * row_tile
    tail = inputs[rows - halo :]
    before = move(tail, "sp", lambda s: s + 2 if s % 2 == 1 and s + 2 < count else None)
    relay = move(before, "sp", lambda s: s - 1 if s % 2 == 1 else None)
    sibling = move(inputs, "sp", lambda s: s ^ 1)
    low = core == 0
    state = jnp.concatenate(
        [jnp.where(low, relay, before), jnp.where(low, inputs, sibling), jnp.where(low, sibling, inputs)], 0
    )
    total = state.shape[0]
    padded = math.ceil(total / lanes) * lanes
    shape = jax.ShapeDtypeStruct
    params = pltpu.CompilerParams(vmem_limit_bytes=16 * 2**20)
    flops = 2 * total * feats * half
    cost = pl.CostEstimate(flops=flops, bytes_accessed=2 * (half * feats + 3 * total * feats), transcendentals=0)

    in_hbm = lambda v: pltpu.with_memory_space_constraint(v, pltpu.HBM)
    deltas = []
    for l in range(layers):
        first, last = l == 0, l == layers - 1
        pieces = [(at, index) for _, at, index in found[2 * l]]
        arrays = [in_hbm(v) for v, _, _ in found[2 * l]]
        outs = [shape((total, half), bf16), shape((8, padded), jnp.float32)]
        if not first:
            outs = [pltpu.HBM((total, feats), bf16)] + outs
        results = pl.pallas_call(
            functools.partial(in_kernel, first, pieces, shard),
            out_shape=outs,
            in_specs=[VMEM] * (1 if first else 3) + [ANY] * len(pieces),
            out_specs=([] if first else [HBM]) + [VMEM] * 2,
            scratch_shapes=[
                pltpu.VMEM((half, feats), bf16),
                pltpu.VMEM((padded, lanes), jnp.float32),
                pltpu.SemaphoreType.DMA((2 * nz,)),
            ]
            + ([] if first else [pltpu.VMEM((total, feats), bf16), pltpu.SemaphoreType.DMA]),
            compiler_params=params,
            cost_estimate=cost,
        )(state, *deltas, *arrays)
        if not first:
            state = results[0]
        partial, squares = results[-2:]
        bits = levels(lax.axis_size("tp"))
        for b, bit in enumerate(bits):
            swap = lambda v: move(v, "tp", lambda s: s ^ bit)
            others = [swap(partial), swap(squares)]
            if b < len(bits) - 1:
                partial, squares = partial + others[0], squares + others[1]
        pieces = [(at, index) for _, at, index in found[2 * l + 1]]
        arrays = [in_hbm(v) for v, _, _ in found[2 * l + 1]]
        operands = (place, partial, others[0], squares, others[1], group, scale[l])
        weights = pltpu.VMEM((half, feats), bf16)
        sems = pltpu.SemaphoreType.DMA((2 * nz,))
        mixed = (total, half)
        call = dict(compiler_params=params, cost_estimate=cost)
        if not last:
            results = [
                pl.pallas_call(
                    functools.partial(out_kernel, pieces, shard, features, halo),
                    out_shape=shape((total, feats), bf16),
                    in_specs=[SMEM] + [VMEM] * 6 + [ANY] * len(pieces),
                    out_specs=VMEM,
                    scratch_shapes=[weights, pltpu.VMEM(mixed, bf16), sems],
                    **call,
                )(*operands, *arrays)
            ]
        else:
            mixed = pl.pallas_call(
                functools.partial(pool_kernel, features, halo),
                out_shape=shape(mixed, bf16),
                in_specs=[SMEM] + [VMEM] * 6,
                out_specs=VMEM,
                **call,
            )(*operands)
            results = pl.pallas_call(
                functools.partial(last_kernel, pieces, shard, halo),
                out_shape=[shape((rows, feats), jnp.float32), shape((rows, feats), bf16)],
                in_specs=[SMEM, VMEM, HBM] + [ANY] * len(pieces),
                out_specs=[VMEM] * 2,
                scratch_shapes=[weights, pltpu.VMEM((rows, feats), bf16), sems, pltpu.SemaphoreType.DMA],
                **call,
            )(place, mixed, in_hbm(state), *arrays)
        deltas = [results[0], move(results[-1], "sp", lambda s: s ^ 1)]

    return (deltas[0] + deltas[1].astype(jnp.float32)).astype(bf16)


def solution(mesh):
    placed = (P("sp", "tp"), P(), P(None, "tp", "sp"), P(), P(None, "sp", "tp"))

    return jax.shard_map(body, mesh=mesh, in_specs=placed, out_specs=P("sp", "tp"), check_vma=False)
```

```python
import functools
import math

import jax
import jax.numpy as jnp
import numpy as np
from jax import lax
from jax.experimental import pallas as pl
from jax.experimental.pallas import tpu as pltpu
from jax.sharding import PartitionSpec as P


epsilon = 1e-06
z_from = 4
window = 16
group_count = 4
lanes = 128
row_tile = 16


VMEM = pl.BlockSpec(memory_space=pltpu.VMEM)
SMEM = pl.BlockSpec(memory_space=pltpu.SMEM)
ANY = pl.BlockSpec(memory_space=pl.ANY)
HBM = pl.BlockSpec(memory_space=pltpu.HBM)


def move(value, axis, target):
    pairs = [(s, target(s)) for s in range(lax.axis_size(axis))]
    return lax.ppermute(value, axis, [(s, t) for s, t in pairs if t is not None])


def levels(nz):
    return [1 << b for b in range(nz.bit_length() - 1)]


def next_hop(z, m, step):
    at = z % (2 * m)
    if step == 0:
        return z + 1 if at == m - 1 else z - 1 if at == m else None
    return z - 1 if at == m - step else z + 1 if at == m - 1 + step else None


def order_table(nz):
    table = [[z] for z in range(nz)]
    for m in levels(nz):
        edge = lambda z: z - z % (2 * m) + (m if z % (2 * m) < m else m - 1)
        table = [table[z] + table[edge(z)] for z in range(nz)]
    return table


def across(value):
    return move(value, "sp", lambda s: s ^ 2)


def level(value, m):
    at = lax.axis_index("sp") // 4 % (2 * m)
    steps = jnp.where(at < m, m - 1 - at, at - m)

    def hop(v, step):
        def target(s):
            z = next_hop(s // 4, m, step)
            return None if z is None else 4 * z + s % 4

        return move(v, "sp", target)

    far = got = hop(value, 0)
    for t in range(1, m):
        got = hop(got, t)
        far = jnp.where(steps == t, got, far)
    return far


def lower(stack, nz):
    arrived, near = [], stack
    for m in levels(nz)[:-1]:
        far = level(near, m)
        arrived.append((far, list(range(m, 2 * m))))
        near = jnp.concatenate([near, far], 1)
    return arrived


def gather(own, opposite, arrived, crossed, nz, split):
    half = nz // 2
    pick = lambda e: e[0] if e[2] is None else e[0][e[2]]
    join = lambda parts: (jnp.concatenate([pick(e) for e in parts], 0), sum([e[1] for e in parts], []), None)
    near = [(own, [0], None)] + arrived
    beyond = [opposite] + crossed
    if not split:
        near = [join(near)]
    far = [(level(pick(e), half), [q + half for q in e[1]], None) for e in near]
    return near + far + beyond + [(across(v), [q + nz for q in at], -1) for v, at, _ in far]


def load_weight(pieces, refs, shard, w, sems):
    copies = []
    for (places, index), ref in zip(pieces, refs):
        for k, place in enumerate(places):
            rows = pl.ds(k * shard, shard)
            copies.append(
                pltpu.make_async_copy(
                    ref.at[rows] if index in (None, -1) else ref.at[index, rows],
                    w.at[pl.ds(place * shard, shard)],
                    sems.at[len(copies)],
                )
            )
    for copy in copies:
        copy.start()
    return copies


def in_kernel(first, pieces, shard, *refs):
    refs = list(refs)
    state = refs.pop(0)
    deltas = [] if first else [refs.pop(0), refs.pop(0)]
    arrays = [refs.pop(0) for _ in pieces]
    kept = None if first else refs.pop(0)
    out, squares, w, sq, sems = refs[:5]
    fresh = state if first else refs[5]
    copies = load_weight(pieces, arrays, shard, w, sems)
    rows = state.shape[0]
    tile = 5 * row_tile if rows % (5 * row_tile) == 0 else row_tile

    @pl.loop(0, rows // tile)
    def _(i):
        at = pl.ds(pl.multiple_of(i * tile, row_tile), tile)
        value = state[at, :].astype(jnp.float32)
        if not first:
            value = value + (deltas[0][at, :].astype(jnp.float32) + deltas[1][at, :].astype(jnp.float32))
            rounded = value.astype(jnp.bfloat16)
            fresh[at, :] = rounded
            value = rounded.astype(jnp.float32)
        total = jnp.sum(value * value, axis=1, keepdims=True)
        sq[at, :] = jnp.broadcast_to(total, (tile, lanes))

    if not first:
        keep = pltpu.make_async_copy(fresh, kept, refs[6])
        keep.start()
    if rows < sq.shape[0]:
        sq[rows:, :] = jnp.zeros((sq.shape[0] - rows, lanes), jnp.float32)
    squares[...] = sq[...].T[: squares.shape[0], :]
    for copy in copies:
        copy.wait()
    step = min(256, w.shape[0])
    for n in range(0, w.shape[0], step):
        out[:, n : n + step] = lax.dot_general(
            fresh[...], w[n : n + step, :], (((1,), (1,)), ((), ())), preferred_element_type=jnp.float32
        ).astype(jnp.bfloat16)
    if not first:
        keep.wait()


def pool(place, own, other, sq_own, sq_other, group, scale, mixed, features, halo):
    rows, width = own.shape
    inv = lax.rsqrt((sq_own[...] + sq_other[...]) / features + epsilon)
    inv = jnp.broadcast_to(inv[:1, :], (lanes, inv.shape[1])).T[:rows, :]
    position = place[0] - halo + lax.broadcasted_iota(jnp.int32, (rows, lanes), 0)
    inv = jnp.where(position >= 0, inv, 0.0)
    for n in range(0, width, lanes):
        at = slice(n, n + lanes)
        value = (own[:, at].astype(jnp.float32) + other[:, at].astype(jnp.float32)) * inv
        value = value.astype(jnp.bfloat16).astype(jnp.float32)
        kind = jnp.broadcast_to(group[:1, at], (rows, lanes))
        sums, running, shift = [], value, 1
        while shift < window:
            running = running + pltpu.roll(running, shift, 0)
            sums.append(running)
            shift *= 2
        total = sums[-1]
        for g in range(group_count - 1):
            total = jnp.where(kind == g, sums[g], total)
        length = jnp.left_shift(jnp.int32(2), kind)
        divisor = jnp.maximum(jnp.minimum(position + 1, length), 1).astype(jnp.float32)
        means = total / divisor - value
        mixed[:, at] = (means * scale[:1, at]).astype(jnp.bfloat16)


def pool_kernel(features, halo, *refs):
    pool(*refs, features, halo)


def out_kernel(pieces, shard, features, halo, *refs):
    operands, arrays = refs[:7], refs[7 : 7 + len(pieces)]
    out, w, mixed, sems = refs[7 + len(pieces) :]
    copies = load_weight(pieces, arrays, shard, w, sems)
    pool(*operands, mixed, features, halo)
    for copy in copies:
        copy.wait()
    step = min(256, w.shape[1])

    @pl.loop(0, w.shape[1] // step)
    def _(i):
        at = pl.ds(pl.multiple_of(i * step, step), step)
        out[:, at] = jnp.dot(mixed[...], w[:, at], preferred_element_type=jnp.float32).astype(jnp.bfloat16)


def last_kernel(pieces, shard, halo, *refs):
    place, mixed, state = refs[:3]
    arrays = refs[3 : 3 + len(pieces)]
    mine, theirs, w, kept, sems, kept_sem = refs[3 + len(pieces) :]
    copies = load_weight(pieces, arrays, shard, w, sems)
    count = mine.shape[0]
    here, there = [
        pl.ds(pl.multiple_of(halo + c * count, row_tile), count) for c in (place[1], 1 - place[1])
    ]
    keep = pltpu.make_async_copy(state.at[here], kept, kept_sem)
    keep.start()
    for copy in copies + [keep]:
        copy.wait()
    step = min(256, w.shape[1])

    @pl.loop(0, w.shape[1] // step)
    def _(i):
        at = pl.ds(pl.multiple_of(i * step, step), step)
        theirs[:, at] = jnp.dot(mixed[there, :], w[:, at], preferred_element_type=jnp.float32).astype(jnp.bfloat16)
        value = jnp.dot(mixed[here, :], w[:, at], preferred_element_type=jnp.float32)
        mine[:, at] = value + kept[:, at].astype(jnp.float32)


def body(inputs, norm_gain, in_weight, pool_scale, out_weight):
    rows, feats = inputs.shape
    layers, _, shard = in_weight.shape
    count = lax.axis_size("sp")
    nz = count // 4
    channels = shard * count
    half = channels // 2
    features = norm_gain.shape[1]
    bf16 = jnp.bfloat16
    here = lax.axis_index("sp")
    core = here % 2

    gain = lax.dynamic_slice_in_dim(norm_gain, lax.axis_index("tp") * feats, feats, 1)
    in_t = (jnp.swapaxes(in_weight, 1, 2).astype(jnp.float32) * gain[:, None, :]).astype(bf16)
    in_opposite = across(in_t)
    found = [None] * (2 * layers)

    def gather_group(stack, matrices, arrived):
        for j, k in enumerate(matrices):
            l = k // 2
            mine = [(v, at, j) for v, at in arrived]
            opposite = (across(out_weight[l]), [nz], None) if k % 2 else (in_opposite, [nz], l)
            if k < z_from:
                crossed = [(across(v[j]), at) for v, at in arrived]
            else:
                whole = opposite[0][l : l + 1] if k % 2 == 0 else opposite[0][None]
                crossed = [(v[0], at) for v, at in lower(whole, nz)]
            crossed = [(v, [q + nz for q in at], None) for v, at in crossed]
            found[k] = gather(stack[j], opposite, mine, crossed, nz, k == 0)

    gather_group(in_t[:1], [0], lower(in_t[:1], nz))
    gather_group(out_weight[:1], [1], lower(out_weight[:1], nz))
    gather_group(in_t[1:], list(range(2, 2 * layers, 2)), lower(in_t[1:], nz))
    later = lower(out_weight[1:], nz)

    order = order_table(nz)
    table = [[(order[s // 4][b % nz] * 2 + ((s // 2) % 2 ^ (b // nz))) * 2 + s % 2 for b in range(2 * nz)] for s in range(count)]
    shards = jnp.asarray(np.array(table, np.int32))[here]
    channel = (shards[:, None] * shard + jnp.arange(shard, dtype=jnp.int32)[None, :]).reshape(1, half)
    group = jnp.broadcast_to(channel // (channels // group_count), (8, half))
    scale = pool_scale.reshape(layers, count, shard)[:, shards].reshape(layers, 1, half)
    scale = jnp.broadcast_to(scale, (layers, 8, half))
    place = jnp.stack([(here // 2) * 2 * rows, core]).astype(jnp.int32)

    halo = math.ceil(layers * (window - 1) / row_tile) * row_tile
    tail = inputs[rows - halo :]
    before = move(tail, "sp", lambda s: s + 2 if s % 2 == 1 and s + 2 < count else None)
    relay = move(before, "sp", lambda s: s - 1 if s % 2 == 1 else None)
    sibling = move(inputs, "sp", lambda s: s ^ 1)
    low = core == 0
    state = jnp.concatenate(
        [jnp.where(low, relay, before), jnp.where(low, inputs, sibling), jnp.where(low, sibling, inputs)], 0
    )
    total = state.shape[0]
    padded = math.ceil(total / lanes) * lanes
    shape = jax.ShapeDtypeStruct
    params = pltpu.CompilerParams(vmem_limit_bytes=16 * 2**20)
    flops = 2 * total * feats * half
    cost = pl.CostEstimate(flops=flops, bytes_accessed=2 * (half * feats + 3 * total * feats), transcendentals=0)

    in_hbm = lambda v: pltpu.with_memory_space_constraint(v, pltpu.HBM)
    deltas = []
    for l in range(layers):
        first, last = l == 0, l == layers - 1
        pieces = [(at, index) for _, at, index in found[2 * l]]
        arrays = [v if i == -1 else in_hbm(v) for v, _, i in found[2 * l]]
        outs = [shape((total, half), bf16), shape((8, padded), jnp.float32)]
        if not first:
            outs = [pltpu.HBM((total, feats), bf16)] + outs
        results = pl.pallas_call(
            functools.partial(in_kernel, first, pieces, shard),
            out_shape=outs,
            in_specs=[VMEM] * (1 if first else 3) + [ANY] * len(pieces),
            out_specs=([] if first else [HBM]) + [VMEM] * 2,
            scratch_shapes=[
                pltpu.VMEM((half, feats), bf16),
                pltpu.VMEM((padded, lanes), jnp.float32),
                pltpu.SemaphoreType.DMA((2 * nz,)),
            ]
            + ([] if first else [pltpu.VMEM((total, feats), bf16), pltpu.SemaphoreType.DMA]),
            compiler_params=params,
            cost_estimate=cost,
        )(state, *deltas, *arrays)
        if not first:
            state = results[0]
        partial, squares = results[-2:]
        if first:
            partial, *held = lax.optimization_barrier([partial] + [v for v, _ in later])
            later = [(v, at) for v, (_, at) in zip(held, later)]
            gather_group(out_weight[1:], list(range(3, 2 * layers, 2)), later)
        bits = levels(lax.axis_size("tp"))
        for b, bit in enumerate(bits):
            swap = lambda v: move(v, "tp", lambda s: s ^ bit)
            others = [swap(partial), swap(squares)]
            if b < len(bits) - 1:
                partial, squares = partial + others[0], squares + others[1]
        pieces = [(at, index) for _, at, index in found[2 * l + 1]]
        arrays = [v if i == -1 else in_hbm(v) for v, _, i in found[2 * l + 1]]
        operands = (place, partial, others[0], squares, others[1], group, scale[l])
        weights = pltpu.VMEM((half, feats), bf16)
        sems = pltpu.SemaphoreType.DMA((2 * nz,))
        mixed = (total, half)
        call = dict(compiler_params=params, cost_estimate=cost)
        if not last:
            results = [
                pl.pallas_call(
                    functools.partial(out_kernel, pieces, shard, features, halo),
                    out_shape=shape((total, feats), bf16),
                    in_specs=[SMEM] + [VMEM] * 6 + [ANY] * len(pieces),
                    out_specs=VMEM,
                    scratch_shapes=[weights, pltpu.VMEM(mixed, bf16), sems],
                    **call,
                )(*operands, *arrays)
            ]
        else:
            mixed = pl.pallas_call(
                functools.partial(pool_kernel, features, halo),
                out_shape=shape(mixed, bf16),
                in_specs=[SMEM] + [VMEM] * 6,
                out_specs=VMEM,
                **call,
            )(*operands)
            results = pl.pallas_call(
                functools.partial(last_kernel, pieces, shard, halo),
                out_shape=[shape((rows, feats), jnp.float32), shape((rows, feats), bf16)],
                in_specs=[SMEM, VMEM, HBM] + [ANY] * len(pieces),
                out_specs=[VMEM] * 2,
                scratch_shapes=[weights, pltpu.VMEM((rows, feats), bf16), sems, pltpu.SemaphoreType.DMA],
                **call,
            )(place, mixed, in_hbm(state), *arrays)
        deltas = [results[0], move(results[-1], "sp", lambda s: s ^ 1)]

    return (deltas[0] + deltas[1].astype(jnp.float32)).astype(bf16)


def solution(mesh):
    placed = (P("sp", "tp"), P(), P(None, "tp", "sp"), P(), P(None, "sp", "tp"))

    return jax.shard_map(body, mesh=mesh, in_specs=placed, out_specs=P("sp", "tp"), check_vma=False)
```

```python
import functools
import math

import jax
import jax.numpy as jnp
import numpy as np
from jax import lax
from jax.experimental import pallas as pl
from jax.experimental.pallas import tpu as pltpu
from jax.sharding import PartitionSpec as P


epsilon = 1e-06
z_from = 4
window = 16
group_count = 4
lanes = 128
row_tile = 16


VMEM = pl.BlockSpec(memory_space=pltpu.VMEM)
SMEM = pl.BlockSpec(memory_space=pltpu.SMEM)
ANY = pl.BlockSpec(memory_space=pl.ANY)
HBM = pl.BlockSpec(memory_space=pltpu.HBM)


def move(value, axis, target):
    pairs = [(s, target(s)) for s in range(lax.axis_size(axis))]
    return lax.ppermute(value, axis, [(s, t) for s, t in pairs if t is not None])


def levels(nz):
    return [1 << b for b in range(nz.bit_length() - 1)]


def next_hop(z, m, step):
    at = z % (2 * m)
    if step == 0:
        return z + 1 if at == m - 1 else z - 1 if at == m else None
    return z - 1 if at == m - step else z + 1 if at == m - 1 + step else None


def order_table(nz):
    table = [[z] for z in range(nz)]
    for m in levels(nz):
        edge = lambda z: z - z % (2 * m) + (m if z % (2 * m) < m else m - 1)
        table = [table[z] + table[edge(z)] for z in range(nz)]
    return table


def across(value):
    return move(value, "sp", lambda s: s ^ 2)


def level(value, m):
    at = lax.axis_index("sp") // 4 % (2 * m)
    steps = jnp.where(at < m, m - 1 - at, at - m)

    def hop(v, step):
        def target(s):
            z = next_hop(s // 4, m, step)
            return None if z is None else 4 * z + s % 4

        return move(v, "sp", target)

    far = got = hop(value, 0)
    for t in range(1, m):
        got = hop(got, t)
        far = jnp.where(steps == t, got, far)
    return far


def lower(stack, nz):
    arrived, near = [], stack
    for m in levels(nz)[:-1]:
        far = level(near, m)
        arrived.append((far, list(range(m, 2 * m))))
        near = jnp.concatenate([near, far], 1)
    return arrived


def gather(own, opposite, arrived, crossed, nz, split):
    half = nz // 2
    pick = lambda e: e[0] if e[2] is None else e[0][e[2]]
    join = lambda parts: (jnp.concatenate([pick(e) for e in parts], 0), sum([e[1] for e in parts], []), None)
    near = [(own, [0], None)] + arrived
    beyond = [opposite] + crossed
    if not split:
        near = [join(near)]
    far = [(level(pick(e), half), [q + half for q in e[1]], None) for e in near]
    return near + far + beyond + [(across(v), [q + nz for q in at], -1) for v, at, _ in far]


def load_weight(pieces, refs, shard, w, sems):
    copies = []
    for (places, index), ref in zip(pieces, refs):
        for k, place in enumerate(places):
            rows = pl.ds(k * shard, shard)
            copies.append(
                pltpu.make_async_copy(
                    ref.at[rows] if index in (None, -1) else ref.at[index, rows],
                    w.at[pl.ds(place * shard, shard)],
                    sems.at[len(copies)],
                )
            )
    for copy in copies:
        copy.start()
    return copies


def in_kernel(first, pieces, shard, *refs):
    refs = list(refs)
    state = refs.pop(0)
    deltas = [] if first else [refs.pop(0), refs.pop(0)]
    arrays = [refs.pop(0) for _ in pieces]
    kept = None if first else refs.pop(0)
    out, squares, w, sq, sems = refs[:5]
    fresh = state if first else refs[5]
    copies = load_weight(pieces, arrays, shard, w, sems)
    rows = out.shape[0]
    skip = state.shape[0] - rows
    tile = 5 * row_tile

    def update(start, count):
        at = pl.ds(start, count)
        value = state[pl.ds(pl.multiple_of(start + skip, row_tile), count), :].astype(jnp.float32)
        if not first:
            value = value + (deltas[0][at, :].astype(jnp.float32) + deltas[1][at, :].astype(jnp.float32))
            rounded = value.astype(jnp.bfloat16)
            fresh[at, :] = rounded
            value = rounded.astype(jnp.float32)
        total = jnp.sum(value * value, axis=1, keepdims=True)
        sq[at, :] = jnp.broadcast_to(total, (count, lanes))

    @pl.loop(0, rows // tile)
    def _(i):
        update(pl.multiple_of(i * tile, row_tile), tile)

    if rows % tile:
        update(rows - rows % tile, rows % tile)
    if not first:
        keep = pltpu.make_async_copy(fresh, kept, refs[6])
        keep.start()
    if rows < sq.shape[0]:
        sq[rows:, :] = jnp.zeros((sq.shape[0] - rows, lanes), jnp.float32)
    squares[...] = sq[...].T[: squares.shape[0], :]
    for copy in copies:
        copy.wait()
    step = min(256, w.shape[0])
    for n in range(0, w.shape[0], step):
        out[:, n : n + step] = lax.dot_general(
            fresh[...], w[n : n + step, :], (((1,), (1,)), ((), ())), preferred_element_type=jnp.float32
        ).astype(jnp.bfloat16)
    if not first:
        keep.wait()


def pool(place, own, other, sq_own, sq_other, group, scale, mixed, features, halo):
    rows, width = own.shape
    inv = lax.rsqrt((sq_own[...] + sq_other[...]) / features + epsilon)
    inv = jnp.broadcast_to(inv[:1, :], (lanes, inv.shape[1])).T[:rows, :]
    position = place[0] - halo + lax.broadcasted_iota(jnp.int32, (rows, lanes), 0)
    inv = jnp.where(position >= 0, inv, 0.0)
    for n in range(0, width, lanes):
        at = slice(n, n + lanes)
        value = (own[:, at].astype(jnp.float32) + other[:, at].astype(jnp.float32)) * inv
        value = value.astype(jnp.bfloat16).astype(jnp.float32)
        kind = jnp.broadcast_to(group[:1, at], (rows, lanes))
        sums, running, shift = [], value, 1
        while shift < window:
            running = running + pltpu.roll(running, shift, 0)
            sums.append(running)
            shift *= 2
        total = sums[-1]
        for g in range(group_count - 1):
            total = jnp.where(kind == g, sums[g], total)
        length = jnp.left_shift(jnp.int32(2), kind)
        divisor = jnp.maximum(jnp.minimum(position + 1, length), 1).astype(jnp.float32)
        means = total / divisor - value
        mixed[:, at] = (means * scale[:1, at]).astype(jnp.bfloat16)


def pool_kernel(features, halo, *refs):
    pool(*refs, features, halo)


def out_kernel(pieces, shard, features, halo, *refs):
    operands, arrays = refs[:7], refs[7 : 7 + len(pieces)]
    out, w, mixed, sems = refs[7 + len(pieces) :]
    copies = load_weight(pieces, arrays, shard, w, sems)
    pool(*operands, mixed, features, halo)
    for copy in copies:
        copy.wait()
    step = min(256, w.shape[1])
    skip = mixed.shape[0] - out.shape[0]

    @pl.loop(0, w.shape[1] // step)
    def _(i):
        at = pl.ds(pl.multiple_of(i * step, step), step)
        out[:, at] = jnp.dot(mixed[skip:, :], w[:, at], preferred_element_type=jnp.float32).astype(jnp.bfloat16)


def last_kernel(pieces, shard, halo, *refs):
    place, mixed, state = refs[:3]
    arrays = refs[3 : 3 + len(pieces)]
    mine, theirs, w, kept, sems, kept_sem = refs[3 + len(pieces) :]
    copies = load_weight(pieces, arrays, shard, w, sems)
    count = mine.shape[0]
    here, there = [
        pl.ds(pl.multiple_of(halo + c * count, row_tile), count) for c in (place[1], 1 - place[1])
    ]
    keep = pltpu.make_async_copy(state.at[here], kept, kept_sem)
    keep.start()
    for copy in copies + [keep]:
        copy.wait()
    step = min(256, w.shape[1])

    @pl.loop(0, w.shape[1] // step)
    def _(i):
        at = pl.ds(pl.multiple_of(i * step, step), step)
        theirs[:, at] = jnp.dot(mixed[there, :], w[:, at], preferred_element_type=jnp.float32).astype(jnp.bfloat16)
        value = jnp.dot(mixed[here, :], w[:, at], preferred_element_type=jnp.float32)
        mine[:, at] = value + kept[:, at].astype(jnp.float32)


def body(inputs, norm_gain, in_weight, pool_scale, out_weight):
    rows, feats = inputs.shape
    layers, _, shard = in_weight.shape
    count = lax.axis_size("sp")
    nz = count // 4
    channels = shard * count
    half = channels // 2
    features = norm_gain.shape[1]
    bf16 = jnp.bfloat16
    here = lax.axis_index("sp")
    core = here % 2

    gain = lax.dynamic_slice_in_dim(norm_gain, lax.axis_index("tp") * feats, feats, 1)
    in_t = (jnp.swapaxes(in_weight, 1, 2).astype(jnp.float32) * gain[:, None, :]).astype(bf16)
    in_opposite = across(in_t)
    found = [None] * (2 * layers)

    def gather_group(stack, matrices, arrived):
        for j, k in enumerate(matrices):
            l = k // 2
            mine = [(v, at, j) for v, at in arrived]
            opposite = (across(out_weight[l]), [nz], None) if k % 2 else (in_opposite, [nz], l)
            if k < z_from:
                crossed = [(across(v[j]), at) for v, at in arrived]
            else:
                whole = opposite[0][l : l + 1] if k % 2 == 0 else opposite[0][None]
                crossed = [(v[0], at) for v, at in lower(whole, nz)]
            crossed = [(v, [q + nz for q in at], None) for v, at in crossed]
            found[k] = gather(stack[j], opposite, mine, crossed, nz, k == 0)

    gather_group(in_t[:1], [0], lower(in_t[:1], nz))
    gather_group(out_weight[:1], [1], lower(out_weight[:1], nz))
    gather_group(in_t[1:], list(range(2, 2 * layers, 2)), lower(in_t[1:], nz))
    later = lower(out_weight[1:], nz)

    order = order_table(nz)
    table = [[(order[s // 4][b % nz] * 2 + ((s // 2) % 2 ^ (b // nz))) * 2 + s % 2 for b in range(2 * nz)] for s in range(count)]
    shards = jnp.asarray(np.array(table, np.int32))[here]
    channel = (shards[:, None] * shard + jnp.arange(shard, dtype=jnp.int32)[None, :]).reshape(1, half)
    group = jnp.broadcast_to(channel // (channels // group_count), (8, half))
    scale = pool_scale.reshape(layers, count, shard)[:, shards].reshape(layers, 1, half)
    scale = jnp.broadcast_to(scale, (layers, 8, half))
    place = jnp.stack([(here // 2) * 2 * rows, core]).astype(jnp.int32)

    halos = [math.ceil((layers - l) * (window - 1) / row_tile) * row_tile for l in range(layers)]
    tail = inputs[rows - halos[0] :]
    before = move(tail, "sp", lambda s: s + 2 if s % 2 == 1 and s + 2 < count else None)
    relay = move(before, "sp", lambda s: s - 1 if s % 2 == 1 else None)
    sibling = move(inputs, "sp", lambda s: s ^ 1)
    low = core == 0
    state = jnp.concatenate(
        [jnp.where(low, relay, before), jnp.where(low, inputs, sibling), jnp.where(low, sibling, inputs)], 0
    )
    shape = jax.ShapeDtypeStruct
    params = pltpu.CompilerParams(vmem_limit_bytes=16 * 2**20)
    in_hbm = lambda v: pltpu.with_memory_space_constraint(v, pltpu.HBM)
    deltas = []
    for l in range(layers):
        first, last = l == 0, l == layers - 1
        halo = halos[l]
        total = 2 * rows + halo
        padded = math.ceil(total / lanes) * lanes
        flops, moved = 2 * total * feats * half, 2 * (half * feats + 3 * total * feats)
        cost = pl.CostEstimate(flops=flops, bytes_accessed=moved, transcendentals=0)
        pieces = [(at, index) for _, at, index in found[2 * l]]
        arrays = [v if i == -1 else in_hbm(v) for v, _, i in found[2 * l]]
        outs = [shape((total, half), bf16), shape((8, padded), jnp.float32)]
        if not first:
            outs = [pltpu.HBM((total, feats), bf16)] + outs
        results = pl.pallas_call(
            functools.partial(in_kernel, first, pieces, shard),
            out_shape=outs,
            in_specs=[VMEM] * (1 if first else 3) + [ANY] * len(pieces),
            out_specs=([] if first else [HBM]) + [VMEM] * 2,
            scratch_shapes=[
                pltpu.VMEM((half, feats), bf16),
                pltpu.VMEM((padded, lanes), jnp.float32),
                pltpu.SemaphoreType.DMA((2 * nz,)),
            ]
            + ([] if first else [pltpu.VMEM((total, feats), bf16), pltpu.SemaphoreType.DMA]),
            compiler_params=params,
            cost_estimate=cost,
        )(state, *deltas, *arrays)
        if not first:
            state = results[0]
        partial, squares = results[-2:]
        if first:
            partial, *held = lax.optimization_barrier([partial] + [v for v, _ in later])
            later = [(v, at) for v, (_, at) in zip(held, later)]
            gather_group(out_weight[1:], list(range(3, 2 * layers, 2)), later)
        bits = levels(lax.axis_size("tp"))
        for b, bit in enumerate(bits):
            swap = lambda v: move(v, "tp", lambda s: s ^ bit)
            others = [swap(partial), swap(squares)]
            if b < len(bits) - 1:
                partial, squares = partial + others[0], squares + others[1]
        pieces = [(at, index) for _, at, index in found[2 * l + 1]]
        arrays = [v if i == -1 else in_hbm(v) for v, _, i in found[2 * l + 1]]
        operands = (place, partial, others[0], squares, others[1], group, scale[l])
        weights = pltpu.VMEM((half, feats), bf16)
        sems = pltpu.SemaphoreType.DMA((2 * nz,))
        mixed = (total, half)
        call = dict(compiler_params=params, cost_estimate=cost)
        if not last:
            results = [
                pl.pallas_call(
                    functools.partial(out_kernel, pieces, shard, features, halo),
                    out_shape=shape((2 * rows + halos[l + 1], feats), bf16),
                    in_specs=[SMEM] + [VMEM] * 6 + [ANY] * len(pieces),
                    out_specs=VMEM,
                    scratch_shapes=[weights, pltpu.VMEM(mixed, bf16), sems],
                    **call,
                )(*operands, *arrays)
            ]
        else:
            mixed = pl.pallas_call(
                functools.partial(pool_kernel, features, halo),
                out_shape=shape(mixed, bf16),
                in_specs=[SMEM] + [VMEM] * 6,
                out_specs=VMEM,
                **call,
            )(*operands)
            results = pl.pallas_call(
                functools.partial(last_kernel, pieces, shard, halo),
                out_shape=[shape((rows, feats), jnp.float32), shape((rows, feats), bf16)],
                in_specs=[SMEM, VMEM, HBM] + [ANY] * len(pieces),
                out_specs=[VMEM] * 2,
                scratch_shapes=[weights, pltpu.VMEM((rows, feats), bf16), sems, pltpu.SemaphoreType.DMA],
                **call,
            )(place, mixed, in_hbm(state), *arrays)
        deltas = [results[0], move(results[-1], "sp", lambda s: s ^ 1)]

    return (deltas[0] + deltas[1].astype(jnp.float32)).astype(bf16)


def solution(mesh):
    placed = (P("sp", "tp"), P(), P(None, "tp", "sp"), P(), P(None, "sp", "tp"))

    return jax.shard_map(body, mesh=mesh, in_specs=placed, out_specs=P("sp", "tp"), check_vma=False)
```
